32 devices in a mesh: ep: 8 (over z, y), tp: 4 (over x, core).
Axes of the slice: x: 2, y: 2, z: 4, core: 2. Of those that a mesh axis runs over, the one named last changes fastest.
Arguments:
- mix_tokens: bfloat16 [8192, 2048], P(('ep', 'tp')), may hold values from -6 to 6
- mix_gain: bfloat16 [2048], replicated, may hold values from 0.099609375 to 1.8984375
- w_branch: bfloat16 [2048, 2048], P(None, 'tp'), may hold values from -0.125 to 0.125
- w_gate_branch: bfloat16 [2048, 2048], P(None, 'tp'), may hold values from -0.125 to 0.125
- conv_taps: bfloat16 [4, 2048], P(None, 'tp'), may hold values from -3 to 3
- recur_gate_w: bfloat16 [32, 64, 64], P('tp'), may hold values from -0.75 to 0.75
- inject_gate_w: bfloat16 [32, 64, 64], P('tp'), may hold values from -0.75 to 0.75
- decay_logit: float32 [2048], P('tp')
- decay_kick: float32 [8192, 32], P('ep', 'tp'), may hold values from -0.7 to 0
- w_mix_out: bfloat16 [2048, 2048], P('tp'), may hold values from -0.125 to 0.125
- moe_tokens: bfloat16 [4096, 2048], P(('ep', 'tp')), may hold values from -6 to 6
- moe_gain: bfloat16 [2048], replicated, may hold values from 0.099609375 to 1.8984375
- expert_ids: int32 [4096, 2], P(('ep', 'tp')), may hold values from 0 to 7, all different within a row; in each aligned block of 128 rows (0 to 127, 128 to 255, ...) at most 64 rows name the same one
- route_weight: float32 [4096, 2], P(('ep', 'tp')), may hold values from 0.1 to 1
- expert_gate_w: bfloat16 [8, 2048, 1024], P('ep', None, 'tp'), may hold values from -0.125 to 0.125
- expert_up_w: bfloat16 [8, 2048, 1024], P('ep', None, 'tp'), may hold values from -0.125 to 0.125
- expert_down_w: bfloat16 [8, 1024, 2048], P('ep', 'tp'), may hold values from -0.1875 to 0.1875
Outputs:
- mixer_out: bfloat16 [8192, 2048], P(('ep', 'tp'))
- expert_out: bfloat16 [4096, 2048], P(('ep', 'tp'))
The draws below stay inside these ranges and needn't reach their ends.
Inputs may be any that keep to these rules, and one draw needn't show every extreme that they name: `expert_ids`: each row names 2 different experts. In each aligned block of 128 rows (the rows of one device) no expert is named more than 64 times, a bound that some block reaches.
All inputs are finite; a program needn't handle non-finite values.
Results may differ from the reference program's by a relative error of at most 0.015.
Values may be sent and summed in bfloat16 or wider, within the bound.
A program may use at most 128 MiB of HBM per device.

```python
import math
import jax
import jax.numpy as jnp
import numpy as np
from jax import lax

D = 2048
RECURRENT_HEADS = 32
HEAD_DIM = 64
B_WIDTH = 2048
CONV = 4
FF = 1024
TOP_K = 2
MIX_DEV = 256
MOE_DEV = 128
MIXER_TOKENS = 8192
MOE_TOKENS = 4096
EXPERTS = 8
CAP = 64
N_TP = 4


def draw_decay_logit(key, part):
    fast_key, rate_key = jax.random.split(jax.random.fold_in(key, 11))
    share = 0.5
    fast_mask = jax.random.uniform(fast_key, (B_WIDTH,), jnp.float32) < share
    unit_draw = jax.random.uniform(rate_key, (B_WIDTH,), jnp.float32)
    fast_rate = jnp.exp(jnp.log(1.0 / 400.0) + unit_draw * jnp.log(400.0 / 120.0))
    slow_rate = jnp.exp(jnp.log(0.05) + unit_draw * jnp.log(2.0)) / MIXER_TOKENS
    step_rate = jnp.where(fast_mask, fast_rate, slow_rate)
    return (-jnp.log(jnp.expm1(step_rate))).astype(jnp.float32)


def draw_decay_kick(key, part):
    rate_key, location_random_key, size_random_key = jax.random.split(jax.random.fold_in(key, 23), 3)
    blocks = MIXER_TOKENS // MIX_DEV
    per_block = jnp.exp(jnp.log(0.5) + jnp.log(4.0) * jax.random.uniform(rate_key, (blocks, 1), jnp.float32))
    block_offset = jnp.repeat(-0.5 * per_block / MIXER_TOKENS, MIX_DEV, axis=0) * jnp.ones((1, RECURRENT_HEADS), jnp.float32)
    spike_locations = jax.random.randint(location_random_key, (3, RECURRENT_HEADS), 0, MIXER_TOKENS)
    spike_depth = jnp.log(jax.random.uniform(size_random_key, (3, RECURRENT_HEADS), jnp.float32, 0.55, 0.8))
    token_position = jnp.arange(MIXER_TOKENS, dtype=jnp.int32)[:, None]
    spike_events = jnp.zeros((MIXER_TOKENS, RECURRENT_HEADS), jnp.float32)
    for index_value in range(3):
        spike_events = spike_events + jnp.where(token_position == spike_locations[index_value][None, :], spike_depth[index_value][None, :], 0.0)
    return (block_offset + spike_events).astype(jnp.float32)


def shard_levels(rng, extent, cuts, smallest, largest):
    level, own = 1.0, jax.random.fold_in(rng, 6)
    for position, shards_of in cuts:
        steps = jnp.exp(jax.random.uniform(jax.random.fold_in(own, position), (shards_of,), jnp.float32, smallest / len(cuts), largest / len(cuts)))
        level = level * jnp.repeat(steps, extent[position] // shards_of).reshape([-1 if axis == position else 1 for axis in range(len(extent))])
    return level


def assign_block(own_key, own, number, rows, count, top, limit, slope):
    order = jax.random.permutation(own_key, count)
    crowded, ordinary = load_shares(count, rows * top, limit, slope, True), load_shares(count, rows * top, limit, slope, False)
    places = jnp.arange(count)

    def named(tallies, offset_by):
        used = int((tallies > 0).sum())
        fixed = max(1, used // 4)
        shifted = fixed + (places - fixed + offset_by * (used - fixed)) % max(1, count - fixed)
        return jnp.zeros((count,), jnp.int32).at[order[jnp.where(places < fixed, places, shifted)]].set(jnp.asarray(tallies, jnp.int32))

    tallies = jnp.where(number % 4 == 0, named(crowded, number // 4), named(ordinary, number - number // 4 - 1))
    mixed = jax.random.permutation(jax.random.fold_in(own, 3), count)
    donor, receiver = mixed[0:count // 2 * 2:2], mixed[1:count // 2 * 2:2]
    margin = jnp.minimum(tallies[donor] - 1, limit - tallies[receiver]) // 2
    margin = jnp.where((donor == order[0]) | (receiver == order[0]) | (tallies[receiver] == 0), 0, jnp.maximum(margin, 0))
    shifted = jax.random.randint(jax.random.fold_in(own, 4), (count // 2,), 0, 1 << 20) % (margin + 1)
    tallies = tallies.at[donor].add(-shifted).at[receiver].add(shifted)
    labels = jnp.searchsorted(jnp.cumsum(tallies), jnp.arange(rows * top), side="right").astype(jnp.int32)
    grid = labels.reshape(top, rows).T
    grid = grid[jax.random.permutation(jax.random.fold_in(own, 1), rows)]
    offset_by = jax.random.randint(jax.random.fold_in(own, 2), (rows, 1), 0, top)
    return jnp.take_along_axis(grid, (jnp.arange(top)[None, :] + offset_by) % top, axis=1)


def load_shares(number_of, total, bound, slope, full):
    weights = [(1 << 20) // math.isqrt(rank ** slope) + 1 for rank in range(1, number_of + 1)]
    largest = bound if full else min(bound, max(-(-total // number_of), total * weights[0] // sum(weights)))
    least = 1 if total - largest >= number_of - 1 else 0
    counts, spare = [largest] + [least] * (number_of - 1), total - largest - least * (number_of - 1)
    while spare > 0:
        candidates = [i for i in range(1, number_of) if counts[i] < largest] or [i for i in range(1, number_of) if counts[i] < bound]
        pool, left = sum([weights[i] for i in candidates]), spare
        for i in candidates:
            addition = min(bound - counts[i], max(1, left * weights[i] // pool), spare)
            counts[i] = counts[i] + addition
            spare = spare - addition
    return np.array(counts)


def centred(own_key, extent, width, bound, pieces=(), kind=jnp.bfloat16):
    drawn = jax.random.normal(own_key, extent, jnp.float32) * width
    if len(pieces) > 0:
        drawn = shard_levels(own_key, extent, pieces, -0.22, 0.18) * drawn
    return jnp.clip(drawn, min=-bound, max=bound).astype(kind)


def setup_inputs(seed: int = 0) -> dict:
    streams_of = jax.random.split(jax.random.key(seed), 18)
    mix_tokens = centred(streams_of[0], (MIXER_TOKENS, D), 1.0, 6.0, ((0, 32),))
    mix_gain = jnp.clip(1.0 + 0.18 * jax.random.normal(streams_of[1], (D,), jnp.float32), 0.099609375, 1.8984375).astype(jnp.bfloat16)
    w_branch = centred(streams_of[2], (D, B_WIDTH), D ** -0.5, 0.125, ((1, 4),))
    w_gate_branch = centred(streams_of[3], (D, B_WIDTH), D ** -0.5, 0.125, ((1, 4),))
    conv_taps = centred(streams_of[4], (CONV, B_WIDTH), CONV ** -0.5, 3.0, ((1, 4),))
    recur_gate_w = centred(streams_of[5], (RECURRENT_HEADS, HEAD_DIM, HEAD_DIM), HEAD_DIM ** -0.5, 0.75, ((0, 4),))
    inject_gate_w = centred(streams_of[6], (RECURRENT_HEADS, HEAD_DIM, HEAD_DIM), HEAD_DIM ** -0.5, 0.75, ((0, 4),))
    decay_logit = draw_decay_logit(jax.random.fold_in(streams_of[17], 71), 0)
    decay_kick = draw_decay_kick(jax.random.fold_in(streams_of[17], 71), 0)
    w_mix_out = centred(streams_of[9], (B_WIDTH, D), B_WIDTH ** -0.5, 0.125, ((0, 4),))
    moe_tokens = centred(streams_of[10], (MOE_TOKENS, D), 1.0, 6.0, ((0, 32),))
    moe_gain = jnp.clip(1.0 + 0.18 * jax.random.normal(streams_of[11], (D,), jnp.float32), 0.099609375, 1.8984375).astype(jnp.bfloat16)
    expert_ids_keys = jax.random.split(jax.random.fold_in(streams_of[12], 1), MOE_TOKENS // MOE_DEV)
    expert_ids_turns = jax.random.permutation(jax.random.fold_in(streams_of[12], 3), MOE_TOKENS // MOE_DEV)
    expert_ids = jax.vmap(lambda own, number: assign_block(jax.random.fold_in(streams_of[12], 2), own, number, MOE_DEV, EXPERTS, TOP_K, CAP, 1))(expert_ids_keys, expert_ids_turns).reshape((MOE_TOKENS, TOP_K))
    route_weight = jnp.clip(jnp.exp(math.log(1.0) - 2.3025851 * jax.random.uniform(streams_of[13], (MOE_TOKENS, TOP_K), jnp.float32) ** shard_levels(streams_of[13], (MOE_TOKENS, TOP_K), ((0, 32),), -0.2, 0.2)), 0.1, 1.0)
    expert_gate_w = centred(streams_of[14], (EXPERTS, D, FF), D ** -0.5, 0.125, ((0, 8), (2, 4)))
    expert_up_w = centred(streams_of[15], (EXPERTS, D, FF), D ** -0.5, 0.125, ((0, 8), (2, 4)))
    expert_down_w = centred(streams_of[16], (EXPERTS, FF, D), FF ** -0.5, 0.1875, ((0, 8), (1, 4)))
    return dict(mix_tokens=mix_tokens, mix_gain=mix_gain, w_branch=w_branch, w_gate_branch=w_gate_branch, conv_taps=conv_taps, recur_gate_w=recur_gate_w, inject_gate_w=inject_gate_w, decay_logit=decay_logit, decay_kick=decay_kick, w_mix_out=w_mix_out, moe_tokens=moe_tokens, moe_gain=moe_gain, expert_ids=expert_ids, route_weight=route_weight, expert_gate_w=expert_gate_w, expert_up_w=expert_up_w, expert_down_w=expert_down_w)


epsilon = 1e-06
gate_const = 8.0

def norm_rows(values, gain_vec):
    value_f32 = values.astype(jnp.float32)
    inv_scale = lax.rsqrt(lax.optimization_barrier(jnp.mean(value_f32 * value_f32, axis=-1, keepdims=True)) + epsilon)
    return (value_f32 * inv_scale * gain_vec.astype(jnp.float32)).astype(jnp.bfloat16)

def chain_link(earlier, later):
    return (later[0] * earlier[0], later[0] * earlier[1] + later[1])

def reference(mix_tokens, mix_gain, w_branch, w_gate_branch, conv_taps, recur_gate_w, inject_gate_w, decay_logit, decay_kick, w_mix_out, moe_tokens, moe_gain, expert_ids, route_weight, expert_gate_w, expert_up_w, expert_down_w):
    mixer_in = norm_rows(mix_tokens, mix_gain)
    branch_x = jnp.dot(mixer_in, w_branch, preferred_element_type=jnp.float32).astype(jnp.bfloat16)
    branch_gate = jnp.dot(mixer_in, w_gate_branch, preferred_element_type=jnp.float32).astype(jnp.bfloat16)
    branch_f32 = branch_x.astype(jnp.float32)
    tap_values = conv_taps.astype(jnp.float32)
    padded = jnp.pad(branch_f32, ((CONV - 1, 0), (0, 0)))
    conv_out = tap_values[CONV - 1] * branch_f32
    for index_value in range(CONV - 1):
        conv_out = conv_out + tap_values[index_value] * padded[index_value:index_value + MIXER_TOKENS]
    conv_low = lax.optimization_barrier(conv_out.astype(jnp.bfloat16))
    low_heads = conv_low.astype(jnp.float32).reshape(MIXER_TOKENS, RECURRENT_HEADS, HEAD_DIM)
    recur = jax.nn.sigmoid(jnp.einsum('thi,hij->thj', low_heads, recur_gate_w.astype(jnp.float32)).reshape(MIXER_TOKENS, B_WIDTH))
    inject = jax.nn.sigmoid(jnp.einsum('thi,hij->thj', low_heads, inject_gate_w.astype(jnp.float32)).reshape(MIXER_TOKENS, B_WIDTH))
    slowness = jax.nn.softplus(-decay_logit)
    kick_wide = jnp.repeat(decay_kick, HEAD_DIM, axis=1)
    log_decay = -gate_const * recur * slowness[None, :] + kick_wide
    drive = jnp.sqrt(-jnp.expm1(2.0 * log_decay)) * inject * conv_out
    _, state = lax.associative_scan(chain_link, (jnp.exp(log_decay), drive), axis=0)
    mixed = (state * jax.nn.gelu(branch_gate.astype(jnp.float32))).astype(jnp.bfloat16)
    col_count = B_WIDTH // N_TP
    summed = jnp.zeros((MIXER_TOKENS, D), jnp.float32)
    for group in range(N_TP):
        piece = jnp.dot(mixed[:, group * col_count:(group + 1) * col_count], w_mix_out[group * col_count:(group + 1) * col_count], preferred_element_type=jnp.float32)
        summed = summed + lax.optimization_barrier(piece.astype(jnp.bfloat16)).astype(jnp.float32)
    mixer_out = summed.astype(jnp.bfloat16)
    moe_in = norm_rows(moe_tokens, moe_gain)
    blocks = MOE_TOKENS // MOE_DEV
    route_ids = expert_ids.reshape(blocks, MOE_DEV * TOP_K)
    onehot = (route_ids[:, :, None] == jnp.arange(EXPERTS, dtype=jnp.int32)[None, None, :]).astype(jnp.int32)
    earlier_count = jnp.cumsum(onehot, axis=1) - onehot
    slot_index = lax.optimization_barrier(jnp.sum(earlier_count * onehot, axis=2))
    per_expert = blocks * CAP
    slot_target = (route_ids * per_expert + jnp.arange(blocks, dtype=jnp.int32)[:, None] * CAP + slot_index).reshape(-1).astype(jnp.int32)
    source = jnp.repeat(moe_in, TOP_K, axis=0)
    buffer = jnp.zeros((EXPERTS * per_expert, D), jnp.bfloat16).at[slot_target].set(source)
    quarter = FF // N_TP

    def run_expert(operands):
        expert_rows, gate_mat, up_mat, down_mat = operands
        hidden = (jax.nn.silu(jnp.dot(expert_rows, gate_mat, preferred_element_type=jnp.float32)) * jnp.dot(expert_rows, up_mat, preferred_element_type=jnp.float32)).astype(jnp.bfloat16)
        summed_rows = jnp.zeros((expert_rows.shape[0], D), jnp.float32)
        for group in range(N_TP):
            piece = jnp.dot(hidden[:, group * quarter:(group + 1) * quarter], down_mat[group * quarter:(group + 1) * quarter], preferred_element_type=jnp.float32)
            summed_rows = summed_rows + lax.optimization_barrier(piece.astype(jnp.bfloat16)).astype(jnp.float32)
        return summed_rows.astype(jnp.bfloat16)
    results = lax.map(run_expert, (buffer.reshape(EXPERTS, per_expert, D), expert_gate_w, expert_up_w, expert_down_w))
    results = results.reshape(EXPERTS * per_expert, D)
    picked = results[slot_target].astype(jnp.float32).reshape(MOE_TOKENS, TOP_K, D)
    expert_out = lax.optimization_barrier(jnp.sum(picked * route_weight[:, :, None], axis=1)).astype(jnp.bfloat16)
    return (mixer_out, expert_out)
```

```python
import functools

import jax
import jax.numpy as jnp
from jax import lax
from jax.experimental import pallas as pl
from jax.experimental.pallas import tpu as pltpu
from jax.sharding import PartitionSpec as P

epsilon = 1e-06
gate_const = 8.0


def norm_rows(values, gain_vec):
    value_f32 = values.astype(jnp.float32)
    inv_scale = lax.rsqrt(jnp.mean(value_f32 * value_f32, axis=-1, keepdims=True) + epsilon)
    return (value_f32 * inv_scale * gain_vec.astype(jnp.float32)).astype(jnp.bfloat16)


MESH = pl.DeviceIdType.MESH
LANES = 128
SEGMENTS = 8
EDGE = 16


def chunk_gates(rows, chunk, prev, x_ref, maps_ref, taps_ref, slow_ref, kick_ref, a_s, b_s):
    start = pl.multiple_of(chunk * rows, rows)
    here = x_ref[pl.ds(start, rows), :].astype(jnp.float32)
    kick = kick_ref[pl.ds(start, rows), :]
    taps = taps_ref[...]
    tap_count = taps.shape[0]
    groups = maps_ref.shape[0]
    per = kick.shape[1] // groups
    dim = LANES // per
    lane = lax.broadcasted_iota(jnp.int32, (rows, LANES), 1)
    for g in range(groups):
        cols = slice(g * LANES, (g + 1) * LANES)
        x = here[:, cols]
        window = jnp.concatenate([prev[:, cols], x], axis=0)
        conv = taps[tap_count - 1 : tap_count, cols] * x
        for k in range(tap_count - 1):
            conv = conv + taps[k : k + 1, cols] * pltpu.roll(window, tap_count - 1 - k, 0)[EDGE:]
        pre = jnp.dot(
            conv.astype(jnp.bfloat16), maps_ref[g], preferred_element_type=jnp.float32
        )
        recur = jax.nn.sigmoid(pre[:, :LANES])
        inject = jax.nn.sigmoid(pre[:, LANES:])
        wide = kick[:, g * per : g * per + 1]
        for j in range(1, per):
            wide = jnp.where(lane >= j * dim, kick[:, g * per + j : g * per + j + 1], wide)
        log_decay = -gate_const * recur * slow_ref[:, cols] + wide
        decay = jnp.exp(log_decay)
        twice = 2.0 * log_decay
        series = 1.0 + twice * (1.0 / 8.0)
        for m in (7.0, 6.0, 5.0, 4.0, 3.0, 2.0):
            series = 1.0 + twice * (1.0 / m) * series
        lost = jnp.where(twice > -0.5, -twice * series, 1.0 - decay * decay)
        a_s[g, pl.ds(start, rows), :] = decay
        b_s[g, pl.ds(start, rows), :] = jnp.sqrt(lost) * inject * conv


def mixer_kernel(
    n,
    x_ref,
    gate_ref,
    maps_ref,
    taps_ref,
    slow_ref,
    kick_ref,
    out_ref,
    a_s,
    b_s,
    gelu_s,
    enter_s,
    halo_s,
    own_s,
    ends_s,
    halo_send,
    halo_recv,
    end_send,
    end_recv,
):
    me = lax.axis_index("ep")
    total = x_ref.shape[0]
    rows = total // SEGMENTS
    groups = maps_ref.shape[0]
    barrier = pltpu.get_barrier_semaphore()

    @pl.loop(1, n)
    def _(d):
        pl.semaphore_signal(
            barrier, inc=1, device_id={"ep": lax.rem(me + d, n)}, device_id_type=MESH
        )

    def later_chunk(chunk):
        ahead = pl.multiple_of(chunk * rows - EDGE, EDGE)
        prev = x_ref[pl.ds(ahead, EDGE), :].astype(jnp.float32)
        chunk_gates(rows, chunk, prev, x_ref, maps_ref, taps_ref, slow_ref, kick_ref, a_s, b_s)

    pl.loop(1, 2)(later_chunk)
    pl.semaphore_wait(barrier, n - 1)
    halo = pltpu.make_async_remote_copy(
        src_ref=x_ref.at[pl.ds(total - EDGE, EDGE), :],
        dst_ref=halo_s,
        send_sem=halo_send,
        recv_sem=halo_recv,
        device_id={"ep": lax.rem(me + 1, n)},
        device_id_type=MESH,
    )
    halo.start()
    pl.loop(2, SEGMENTS)(later_chunk)
    halo.wait()
    prev = jnp.where(me > 0, halo_s[...].astype(jnp.float32), 0.0)
    chunk_gates(rows, 0, prev, x_ref, maps_ref, taps_ref, slow_ref, kick_ref, a_s, b_s)

    ones = jnp.ones((SEGMENTS, LANES), jnp.float32)
    zeros = jnp.zeros((SEGMENTS, LANES), jnp.float32)

    def one(step, carry):
        after = []
        for g in range(groups):
            prod, state = carry[g]
            at = pl.ds(step, SEGMENTS, stride=rows)
            decay = a_s[g, at, :]
            state = decay * state + b_s[g, at, :]
            prod = decay * prod
            a_s[g, at, :] = prod
            b_s[g, at, :] = state
            after.append((prod, state))
        return tuple(after)

    ends = lax.fori_loop(0, rows, one, tuple((ones, zeros) for _ in range(groups)), unroll=4)

    for g in range(groups):
        prod, state = ends[g]
        p, h = ones[:1], zeros[:1]
        for s in range(SEGMENTS):
            enter_s[0, g, s : s + 1, :] = p
            enter_s[1, g, s : s + 1, :] = h
            h = prod[s : s + 1] * h + state[s : s + 1]
            p = prod[s : s + 1] * p
        own_s[0:1, g * LANES : (g + 1) * LANES] = p
        own_s[1:2, g * LANES : (g + 1) * LANES] = h
    own_s[2:, :] = jnp.zeros_like(own_s[2:, :])
    ends_s[me] = own_s[...]

    def end_copy(sender, target):
        return pltpu.make_async_remote_copy(
            src_ref=own_s,
            dst_ref=ends_s.at[sender],
            send_sem=end_send.at[target],
            recv_sem=end_recv.at[sender],
            device_id={"ep": target},
            device_id_type=MESH,
        )

    @pl.loop(1, n)
    def _(d):
        end_copy(me, lax.rem(me + d, n)).start()

    @pl.loop(0, SEGMENTS)
    def _(c):
        at = pl.ds(pl.multiple_of(c * rows, rows), rows)
        for g in range(groups):
            gate = gate_ref[at, g * LANES : (g + 1) * LANES].astype(jnp.float32)
            gelu_s[g, at, :] = jax.nn.gelu(gate)

    @pl.loop(1, n)
    def _(d):
        end_copy(me, lax.rem(me + d, n)).wait_send()

    @pl.loop(1, n)
    def _(d):
        end_copy(lax.rem(me + d, n), lax.rem(me + d, n)).wait_recv()

    def fold(s, carried):
        pair = ends_s[s]
        return jnp.where(s < me, pair[0:1] * carried + pair[1:2], carried)

    carried = lax.fori_loop(0, n, fold, jnp.zeros((1, groups * LANES), jnp.float32))
    for g in range(groups):
        enter_s[1, g] = enter_s[0, g] * carried[:, g * LANES : (g + 1) * LANES] + enter_s[1, g]

    @pl.loop(0, SEGMENTS)
    def _(c):
        at = pl.ds(pl.multiple_of(c * rows, rows), rows)
        for g in range(groups):
            state = b_s[g, at, :] + a_s[g, at, :] * enter_s[1, g, pl.ds(c, 1), :]
            out_ref[at, g * LANES : (g + 1) * LANES] = (state * gelu_s[g, at, :]).astype(
                out_ref.dtype
            )


def paired_maps(head_maps):
    head_count, head_dim, _ = head_maps.shape
    per = LANES // head_dim
    grouped = head_maps.reshape(head_count // per, per, head_dim, 1, head_dim)
    eye = jnp.eye(per, dtype=head_maps.dtype)[None, :, None, :, None]
    return (grouped * eye).reshape(head_count // per, LANES, LANES)


def run_mixer(
    mix_tokens,
    mix_gain,
    w_branch,
    w_gate_branch,
    conv_taps,
    recur_gate_w,
    inject_gate_w,
    decay_logit,
    decay_kick,
    w_mix_out,
):
    mixer_in = norm_rows(mix_tokens, mix_gain)
    piece = lax.all_gather(mixer_in, "tp", axis=0, tiled=True)
    branch_x = jnp.dot(piece, w_branch, preferred_element_type=jnp.float32).astype(jnp.bfloat16)
    branch_gate = jnp.dot(piece, w_gate_branch, preferred_element_type=jnp.float32).astype(
        jnp.bfloat16
    )
    maps = jnp.concatenate([paired_maps(recur_gate_w), paired_maps(inject_gate_w)], axis=2)
    slowness = jax.nn.softplus(-decay_logit)[None, :]
    n = lax.axis_size("ep")
    row_count, col_count = branch_x.shape
    groups = col_count // LANES
    plane = pltpu.VMEM((groups, row_count, LANES), jnp.float32)
    mixed = pl.pallas_call(
        functools.partial(mixer_kernel, n),
        out_shape=jax.ShapeDtypeStruct((row_count, col_count), jnp.bfloat16),
        in_specs=[pl.BlockSpec(memory_space=pltpu.VMEM)] * 6,
        out_specs=pl.BlockSpec(memory_space=pltpu.VMEM),
        scratch_shapes=[
            plane,
            plane,
            plane,
            pltpu.VMEM((2, groups, SEGMENTS, LANES), jnp.float32),
            pltpu.VMEM((EDGE, col_count), jnp.bfloat16),
            pltpu.VMEM((8, col_count), jnp.float32),
            pltpu.VMEM((n, 8, col_count), jnp.float32),
            pltpu.SemaphoreType.DMA,
            pltpu.SemaphoreType.DMA,
            pltpu.SemaphoreType.DMA((n,)),
            pltpu.SemaphoreType.DMA((n,)),
        ],
        compiler_params=pltpu.CompilerParams(
            collective_id=0, has_side_effects=True, vmem_limit_bytes=24 * 1024 * 1024
        ),
        cost_estimate=pl.CostEstimate(
            flops=100 * row_count * col_count,
            bytes_accessed=40 * row_count * col_count,
            transcendentals=6 * row_count * col_count,
        ),
    )(branch_x, branch_gate, maps, conv_taps.astype(jnp.float32), slowness, decay_kick)
    return lax.psum_scatter(
        jnp.dot(mixed, w_mix_out, preferred_element_type=jnp.float32).astype(jnp.bfloat16),
        "tp",
        scatter_dimension=0,
        tiled=True,
    )


def run_experts(
    moe_tokens, moe_gain, expert_ids, route_weight, expert_gate_w, expert_up_w, expert_down_w
):
    moe_in = norm_rows(moe_tokens, moe_gain)
    local_rows, top_count = expert_ids.shape
    experts = lax.axis_size("ep")
    room = 2 * local_rows * top_count // experts
    flat_ids = expert_ids.reshape(-1)
    onehot = (flat_ids[:, None] == jnp.arange(experts, dtype=jnp.int32)[None, :]).astype(jnp.int32)
    earlier_count = jnp.cumsum(onehot, axis=0) - onehot
    slot_index = jnp.sum(earlier_count * onehot, axis=1)
    slot_target = flat_ids * room + slot_index
    slots_total = experts * room
    slot_table = (slot_target[:, None] == jnp.arange(slots_total, dtype=jnp.int32)[None, :]).astype(
        jnp.bfloat16
    )
    token_of = (
        jnp.arange(local_rows * top_count, dtype=jnp.int32)[None, :] // top_count
        == jnp.arange(local_rows, dtype=jnp.int32)[:, None]
    ).astype(jnp.bfloat16)
    dispatch_table = jnp.dot(token_of, slot_table, preferred_element_type=jnp.float32).astype(
        jnp.bfloat16
    )
    outgoing = jnp.dot(dispatch_table.T, moe_in, preferred_element_type=jnp.float32).astype(
        jnp.bfloat16
    )
    arrived = lax.all_to_all(outgoing, "ep", split_axis=0, concat_axis=0, tiled=True)
    gate_mat = expert_gate_w[0]
    up_mat = expert_up_w[0]
    down_mat = expert_down_w[0]
    full_gate, full_up, full_down = (
        lax.all_gather(gate_mat, "tp", axis=1, tiled=True),
        lax.all_gather(up_mat, "tp", axis=1, tiled=True),
        lax.all_gather(down_mat, "tp", axis=0, tiled=True),
    )
    hidden = (
        jax.nn.silu(jnp.dot(arrived, full_gate, preferred_element_type=jnp.float32))
        * jnp.dot(arrived, full_up, preferred_element_type=jnp.float32)
    ).astype(jnp.bfloat16)
    groups = lax.axis_size("tp")
    quarter = down_mat.shape[0]
    summed_rows = jnp.zeros((arrived.shape[0], full_down.shape[1]), jnp.float32)
    for group in range(groups):
        piece = jnp.dot(
            hidden[:, group * quarter : (group + 1) * quarter],
            full_down[group * quarter : (group + 1) * quarter],
            preferred_element_type=jnp.float32,
        )
        summed_rows = summed_rows + lax.optimization_barrier(piece.astype(jnp.bfloat16)).astype(
            jnp.float32
        )
    expert_done = summed_rows.astype(jnp.bfloat16)
    returned = lax.all_to_all(expert_done, "ep", split_axis=0, concat_axis=0, tiled=True)
    weighted_table = jnp.zeros((local_rows, slots_total), jnp.float32)
    for pick in range(top_count):
        pick_table = (
            slot_target.reshape(local_rows, top_count)[:, pick][:, None]
            == jnp.arange(slots_total, dtype=jnp.int32)[None, :]
        ).astype(jnp.float32)
        weighted_table = weighted_table + pick_table * route_weight[:, pick][:, None]
    combined = jnp.dot(
        weighted_table, returned.astype(jnp.float32), precision=lax.Precision.HIGHEST
    )
    return combined.astype(jnp.bfloat16)


def body(
    mix_tokens,
    mix_gain,
    w_branch,
    w_gate_branch,
    conv_taps,
    recur_gate_w,
    inject_gate_w,
    decay_logit,
    decay_kick,
    w_mix_out,
    moe_tokens,
    moe_gain,
    expert_ids,
    route_weight,
    expert_gate_w,
    expert_up_w,
    expert_down_w,
):
    mixer_out = run_mixer(
        mix_tokens,
        mix_gain,
        w_branch,
        w_gate_branch,
        conv_taps,
        recur_gate_w,
        inject_gate_w,
        decay_logit,
        decay_kick,
        w_mix_out,
    )
    expert_out = run_experts(
        moe_tokens, moe_gain, expert_ids, route_weight, expert_gate_w, expert_up_w, expert_down_w
    )
    return (mixer_out, expert_out)


def solution(mesh):
    placed = (
        P(("ep", "tp"), None),
        P(),
        P(None, "tp"),
        P(None, "tp"),
        P(None, "tp"),
        P("tp", None, None),
        P("tp", None, None),
        P("tp"),
        P("ep", "tp"),
        P("tp", None),
        P(("ep", "tp"), None),
        P(),
        P(("ep", "tp"), None),
        P(("ep", "tp"), None),
        P("ep", None, "tp"),
        P("ep", None, "tp"),
        P("ep", "tp", None),
    )
    return jax.shard_map(
        body,
        mesh=mesh,
        in_specs=placed,
        out_specs=(P(("ep", "tp"), None), P(("ep", "tp"), None)),
        check_vma=False,
    )
```

```python
import functools

import jax
import jax.numpy as jnp
from jax import lax
from jax.experimental import pallas as pl
from jax.experimental.pallas import tpu as pltpu
from jax.sharding import PartitionSpec as P


epsilon = 1e-06
gate_const = 8.0


def norm_rows(values, gain_vec):
    value_f32 = values.astype(jnp.float32)
    inv_scale = lax.rsqrt(jnp.mean(value_f32 * value_f32, axis=-1, keepdims=True) + epsilon)
    return (value_f32 * inv_scale * gain_vec.astype(jnp.float32)).astype(jnp.bfloat16)


MESH = pl.DeviceIdType.MESH
LANES = 128
SEGMENTS = 8
EDGE = 16


def chunk_gates(rows, chunk, prev, x_ref, maps_ref, taps_ref, slow_ref, kick_ref, a_s, b_s):
    start = pl.multiple_of(chunk * rows, rows)
    here = x_ref[pl.ds(start, rows), :].astype(jnp.float32)
    kick = kick_ref[pl.ds(start, rows), :]
    taps = taps_ref[...]
    tap_count = taps.shape[0]
    groups = maps_ref.shape[0]
    per = kick.shape[1] // groups
    dim = LANES // per
    lane = lax.broadcasted_iota(jnp.int32, (rows, LANES), 1)
    for g in range(groups):
        cols = slice(g * LANES, (g + 1) * LANES)
        x = here[:, cols]
        window = jnp.concatenate([prev[:, cols], x], axis=0)
        conv = taps[tap_count - 1 : tap_count, cols] * x
        for k in range(tap_count - 1):
            conv = conv + taps[k : k + 1, cols] * pltpu.roll(window, tap_count - 1 - k, 0)[EDGE:]
        pre = jnp.dot(
            conv.astype(jnp.bfloat16), maps_ref[g], preferred_element_type=jnp.float32
        )
        recur = jax.nn.sigmoid(pre[:, :LANES])
        inject = jax.nn.sigmoid(pre[:, LANES:])
        wide = kick[:, g * per : g * per + 1]
        for j in range(1, per):
            wide = jnp.where(lane >= j * dim, kick[:, g * per + j : g * per + j + 1], wide)
        log_decay = -gate_const * recur * slow_ref[:, cols] + wide
        decay = jnp.exp(log_decay)
        twice = 2.0 * log_decay
        series = 1.0 + twice * (1.0 / 8.0)
        for m in (7.0, 6.0, 5.0, 4.0, 3.0, 2.0):
            series = 1.0 + twice * (1.0 / m) * series
        lost = jnp.where(twice > -0.5, -twice * series, 1.0 - decay * decay)
        a_s[g, pl.ds(start, rows), :] = decay
        b_s[g, pl.ds(start, rows), :] = jnp.sqrt(lost) * inject * conv


def mixer_kernel(
    n,
    x_ref,
    gate_ref,
    maps_ref,
    taps_ref,
    slow_ref,
    kick_ref,
    out_ref,
    a_s,
    b_s,
    gelu_s,
    enter_s,
    halo_s,
    own_s,
    ends_s,
    halo_send,
    halo_recv,
    end_send,
    end_recv,
):
    me = lax.axis_index("ep")
    total = x_ref.shape[0]
    rows = total // SEGMENTS
    groups = maps_ref.shape[0]
    barrier = pltpu.get_barrier_semaphore()

    @pl.loop(1, n)
    def _(d):
        pl.semaphore_signal(
            barrier, inc=1, device_id={"ep": lax.rem(me + d, n)}, device_id_type=MESH
        )

    def later_chunk(chunk):
        ahead = pl.multiple_of(chunk * rows - EDGE, EDGE)
        prev = x_ref[pl.ds(ahead, EDGE), :].astype(jnp.float32)
        chunk_gates(rows, chunk, prev, x_ref, maps_ref, taps_ref, slow_ref, kick_ref, a_s, b_s)

    pl.loop(1, 2)(later_chunk)
    pl.semaphore_wait(barrier, n - 1)
    halo = pltpu.make_async_remote_copy(
        src_ref=x_ref.at[pl.ds(total - EDGE, EDGE), :],
        dst_ref=halo_s,
        send_sem=halo_send,
        recv_sem=halo_recv,
        device_id={"ep": lax.rem(me + 1, n)},
        device_id_type=MESH,
    )
    halo.start()
    pl.loop(2, SEGMENTS)(later_chunk)
    halo.wait()
    prev = jnp.where(me > 0, halo_s[...].astype(jnp.float32), 0.0)
    chunk_gates(rows, 0, prev, x_ref, maps_ref, taps_ref, slow_ref, kick_ref, a_s, b_s)

    ones = jnp.ones((SEGMENTS, LANES), jnp.float32)
    zeros = jnp.zeros((SEGMENTS, LANES), jnp.float32)

    def one(step, carry):
        after = []
        for g in range(groups):
            prod, state = carry[g]
            at = pl.ds(step, SEGMENTS, stride=rows)
            decay = a_s[g, at, :]
            state = decay * state + b_s[g, at, :]
            prod = decay * prod
            a_s[g, at, :] = prod
            b_s[g, at, :] = state
            after.append((prod, state))
        return tuple(after)

    ends = lax.fori_loop(0, rows, one, tuple((ones, zeros) for _ in range(groups)), unroll=4)

    for g in range(groups):
        prod, state = ends[g]
        p, h = ones[:1], zeros[:1]
        for s in range(SEGMENTS):
            enter_s[0, g, s : s + 1, :] = p
            enter_s[1, g, s : s + 1, :] = h
            h = prod[s : s + 1] * h + state[s : s + 1]
            p = prod[s : s + 1] * p
        own_s[0:1, g * LANES : (g + 1) * LANES] = p
        own_s[1:2, g * LANES : (g + 1) * LANES] = h
    own_s[2:, :] = jnp.zeros_like(own_s[2:, :])
    ends_s[me] = own_s[...]

    def end_copy(sender, target):
        return pltpu.make_async_remote_copy(
            src_ref=own_s,
            dst_ref=ends_s.at[sender],
            send_sem=end_send.at[target],
            recv_sem=end_recv.at[sender],
            device_id={"ep": target},
            device_id_type=MESH,
        )

    @pl.loop(1, n)
    def _(d):
        end_copy(me, lax.rem(me + d, n)).start()

    @pl.loop(0, SEGMENTS)
    def _(c):
        at = pl.ds(pl.multiple_of(c * rows, rows), rows)
        for g in range(groups):
            gate = gate_ref[at, g * LANES : (g + 1) * LANES].astype(jnp.float32)
            gelu_s[g, at, :] = jax.nn.gelu(gate)

    @pl.loop(1, n)
    def _(d):
        end_copy(me, lax.rem(me + d, n)).wait_send()

    @pl.loop(1, n)
    def _(d):
        end_copy(lax.rem(me + d, n), lax.rem(me + d, n)).wait_recv()

    def fold(s, carried):
        pair = ends_s[s]
        return jnp.where(s < me, pair[0:1] * carried + pair[1:2], carried)

    carried = lax.fori_loop(0, n, fold, jnp.zeros((1, groups * LANES), jnp.float32))
    for g in range(groups):
        enter_s[1, g] = enter_s[0, g] * carried[:, g * LANES : (g + 1) * LANES] + enter_s[1, g]

    @pl.loop(0, SEGMENTS)
    def _(c):
        at = pl.ds(pl.multiple_of(c * rows, rows), rows)
        for g in range(groups):
            state = b_s[g, at, :] + a_s[g, at, :] * enter_s[1, g, pl.ds(c, 1), :]
            out_ref[at, g * LANES : (g + 1) * LANES] = (state * gelu_s[g, at, :]).astype(
                out_ref.dtype
            )


def paired_maps(head_maps):
    head_count, head_dim, _ = head_maps.shape
    per = LANES // head_dim
    grouped = head_maps.reshape(head_count // per, per, head_dim, 1, head_dim)
    eye = jnp.eye(per, dtype=head_maps.dtype)[None, :, None, :, None]
    return (grouped * eye).reshape(head_count // per, LANES, LANES)


def run_mixer(
    mix_tokens,
    mix_gain,
    w_branch,
    w_gate_branch,
    conv_taps,
    recur_gate_w,
    inject_gate_w,
    decay_logit,
    decay_kick,
    w_mix_out,
):
    mixer_in = norm_rows(mix_tokens, mix_gain)
    piece = lax.all_gather(mixer_in, "tp", axis=0, tiled=True)
    branch_x = jnp.dot(piece, w_branch, preferred_element_type=jnp.float32).astype(jnp.bfloat16)
    branch_gate = jnp.dot(piece, w_gate_branch, preferred_element_type=jnp.float32).astype(
        jnp.bfloat16
    )
    maps = jnp.concatenate([paired_maps(recur_gate_w), paired_maps(inject_gate_w)], axis=2)
    slowness = jax.nn.softplus(-decay_logit)[None, :]
    n = lax.axis_size("ep")
    row_count, col_count = branch_x.shape
    groups = col_count // LANES
    plane = pltpu.VMEM((groups, row_count, LANES), jnp.float32)
    call = pl.pallas_call(
        functools.partial(mixer_kernel, n),
        out_shape=jax.ShapeDtypeStruct((row_count, col_count), jnp.bfloat16),
        in_specs=[pl.BlockSpec(memory_space=pltpu.VMEM)] * 6,
        out_specs=pl.BlockSpec(memory_space=pltpu.VMEM),
        scratch_shapes=[
            plane,
            plane,
            plane,
            pltpu.VMEM((2, groups, SEGMENTS, LANES), jnp.float32),
            pltpu.VMEM((EDGE, col_count), jnp.bfloat16),
            pltpu.VMEM((8, col_count), jnp.float32),
            pltpu.VMEM((n, 8, col_count), jnp.float32),
            pltpu.SemaphoreType.DMA,
            pltpu.SemaphoreType.DMA,
            pltpu.SemaphoreType.DMA((n,)),
            pltpu.SemaphoreType.DMA((n,)),
        ],
        compiler_params=pltpu.CompilerParams(
            collective_id=0, has_side_effects=True, vmem_limit_bytes=24 * 1024 * 1024
        ),
        cost_estimate=pl.CostEstimate(
            flops=100 * row_count * col_count,
            bytes_accessed=40 * row_count * col_count,
            transcendentals=6 * row_count * col_count,
        ),
    )
    taps = conv_taps.astype(jnp.float32)
    mixed = call(branch_x, branch_gate, maps, taps, slowness, decay_kick)
    return lax.psum_scatter(
        jnp.dot(mixed, w_mix_out, preferred_element_type=jnp.float32).astype(jnp.bfloat16),
        "tp",
        scatter_dimension=0,
        tiled=True,
    )


def weight_pieces(own, axis):
    size = lax.axis_size(axis)
    pieces = [own]
    if size & (size - 1):
        for d in range(1, size):
            route = [(i, (i + d) % size) for i in range(size)]
            pieces.append(tuple(lax.ppermute(v, axis, route) for v in own))
        return pieces
    bit = size // 2
    while bit:
        route = [(i, i ^ bit) for i in range(size)]
        sent = []
        for piece in pieces:
            moved = []
            for v in piece:
                moved.append(lax.ppermute(v, axis, route))
            sent.append(tuple(moved))
        pieces += sent
        bit //= 2
    order = [0] + [k for k in range(1, size) if k % 2 == 0] + [k for k in range(1, size) if k % 2]
    return [pieces[k] for k in order]


def run_experts(
    moe_tokens, moe_gain, expert_ids, route_weight, expert_gate_w, expert_up_w, expert_down_w
):
    moe_in = norm_rows(moe_tokens, moe_gain)
    local_rows, top_count = expert_ids.shape
    experts = lax.axis_size("ep")
    room = 2 * local_rows * top_count // experts
    flat_ids = expert_ids.reshape(-1)
    onehot = (flat_ids[:, None] == jnp.arange(experts, dtype=jnp.int32)[None, :]).astype(jnp.int32)
    earlier_count = jnp.cumsum(onehot, axis=0) - onehot
    slot_index = jnp.sum(earlier_count * onehot, axis=1)
    slot_target = flat_ids * room + slot_index
    slots_total = experts * room
    slot_table = (slot_target[:, None] == jnp.arange(slots_total, dtype=jnp.int32)[None, :]).astype(
        jnp.bfloat16
    )
    token_of = (
        jnp.arange(local_rows * top_count, dtype=jnp.int32)[None, :] // top_count
        == jnp.arange(local_rows, dtype=jnp.int32)[:, None]
    ).astype(jnp.bfloat16)
    dispatch_table = jnp.dot(token_of, slot_table, preferred_element_type=jnp.float32).astype(
        jnp.bfloat16
    )
    outgoing = jnp.dot(dispatch_table.T, moe_in, preferred_element_type=jnp.float32).astype(
        jnp.bfloat16
    )
    arrived = lax.all_to_all(outgoing, "ep", split_axis=0, concat_axis=0, tiled=True)
    gate_mat = expert_gate_w[0]
    up_mat = expert_up_w[0]
    down_mat = expert_down_w[0]
    width = gate_mat.shape[1]
    pieces = weight_pieces((jnp.concatenate([gate_mat, up_mat], axis=1), down_mat), "tp")
    summed_rows = None
    for both_mat, down_piece in pieces:
        pre = jnp.dot(arrived, both_mat, preferred_element_type=jnp.float32)
        hidden = (jax.nn.silu(pre[:, :width]) * pre[:, width:]).astype(jnp.bfloat16)
        part = jnp.dot(hidden, down_piece, preferred_element_type=jnp.float32)
        summed_rows = part if summed_rows is None else summed_rows + part
    expert_done = summed_rows.astype(jnp.bfloat16)
    returned = lax.all_to_all(expert_done, "ep", split_axis=0, concat_axis=0, tiled=True)
    weighted_table = jnp.zeros((local_rows, slots_total), jnp.float32)
    for pick in range(top_count):
        pick_table = (
            slot_target.reshape(local_rows, top_count)[:, pick][:, None]
            == jnp.arange(slots_total, dtype=jnp.int32)[None, :]
        ).astype(jnp.float32)
        weighted_table = weighted_table + pick_table * route_weight[:, pick][:, None]
    combined = jnp.dot(
        weighted_table, returned.astype(jnp.float32), precision=lax.Precision.HIGHEST
    )
    return combined.astype(jnp.bfloat16)


def body(
    mix_tokens,
    mix_gain,
    w_branch,
    w_gate_branch,
    conv_taps,
    recur_gate_w,
    inject_gate_w,
    decay_logit,
    decay_kick,
    w_mix_out,
    moe_tokens,
    moe_gain,
    expert_ids,
    route_weight,
    expert_gate_w,
    expert_up_w,
    expert_down_w,
):
    mixer_out = run_mixer(
        mix_tokens,
        mix_gain,
        w_branch,
        w_gate_branch,
        conv_taps,
        recur_gate_w,
        inject_gate_w,
        decay_logit,
        decay_kick,
        w_mix_out,
    )
    expert_out = run_experts(
        moe_tokens, moe_gain, expert_ids, route_weight, expert_gate_w, expert_up_w, expert_down_w
    )
    return (mixer_out, expert_out)


def solution(mesh):
    placed = (
        P(("ep", "tp"), None),
        P(),
        P(None, "tp"),
        P(None, "tp"),
        P(None, "tp"),
        P("tp", None, None),
        P("tp", None, None),
        P("tp"),
        P("ep", "tp"),
        P("tp", None),
        P(("ep", "tp"), None),
        P(),
        P(("ep", "tp"), None),
        P(("ep", "tp"), None),
        P("ep", None, "tp"),
        P("ep", None, "tp"),
        P("ep", "tp", None),
    )

    return jax.shard_map(
        body,
        mesh=mesh,
        in_specs=placed,
        out_specs=(P(("ep", "tp"), None), P(("ep", "tp"), None)),
        check_vma=False,
    )
```
